32 devices in a mesh: sp: 8 (over z, y), tp: 4 (over x, core).
Axes of the slice: x: 2, y: 2, z: 4, core: 2. Of those that a mesh axis runs over, the one named last changes fastest.
Arguments:
- tokens: bfloat16 [3072, 2048], P('sp'), may hold values from -6 to 6
- norm_gain: float32 [2048], replicated, may hold values from 0.1 to 12
- w_query: bfloat16 [3, 512, 2048], P(None, 'tp'), may hold values from -0.125 to 0.125
- w_key: bfloat16 [3, 512, 2048], P(None, 'tp'), may hold values from -0.125 to 0.125
- w_value: bfloat16 [3, 512, 2048], P(None, 'tp'), may hold values from -0.125 to 0.125
- w_out: bfloat16 [512, 2048], P(None, 'tp'), may hold values from -0.25 to 0.25
Outputs:
- projected: bfloat16 [3072, 2048], P('sp', 'tp')
- log_weight: float32 [8, 3072], P('tp', 'sp')
The draws below stay inside these ranges and needn't reach their ends.
All inputs are finite; a program needn't handle non-finite values.
Results may differ from the reference program's by a relative error of at most 0.006.
The reference program's roundings to bfloat16 on the way count: a program that leaves them out, or rounds other values in their place, can miss the bound.
Values may be sent and summed in bfloat16 or wider, within the bound.
A program may use at most 64 MiB of HBM per device.

```python
import math
import jax
import jax.numpy as jnp
from jax import lax

D = 2048
HEAD_DIM = 64
SLOTS = 8
STEPS = 128
MIDDLE_DILATION = 4
WIDE_DILATION = 16
TOK_DEV = 384
TOKENS = 3072


def draw_norm_gain(key, part):
    return 1.0 + 0.18 * jnp.clip(jax.random.normal(key, (D,), jnp.float32), -5.0, 5.0)


def levels(own_key, dims, split, least, largest):
    factor_of, own = 1.0, jax.random.fold_in(own_key, 6)
    for position, parts in split:
        steps = jnp.exp(jax.random.uniform(jax.random.fold_in(own, position), (parts,), jnp.float32, least / len(split), largest / len(split)))
        factor_of = factor_of * jnp.repeat(steps, dims[position] // parts).reshape([-1 if axis == position else 1 for axis in range(len(dims))])
    return factor_of


def gaussian(stream_key, dims, deviation, reach, shards=(), kind=jnp.bfloat16):
    loudness = levels(stream_key, dims, shards, -0.22, 0.18) if shards else 1.0
    array = jax.random.normal(stream_key, dims, jnp.float32) * deviation * loudness
    return jnp.minimum(jnp.maximum(array, -reach), reach).astype(kind)


def setup_inputs(seed: int = 0) -> dict:
    key_list = jax.random.split(jax.random.key(seed), 7)
    tokens = gaussian(key_list[0], (TOKENS, D), 1.0, 6.0, ((0, 8),))
    norm_gain = draw_norm_gain(jax.random.fold_in(key_list[6], 71), 0)
    w_query = gaussian(key_list[2], (3, SLOTS * HEAD_DIM, D), D ** -0.5, 0.125, ((1, 4),))
    w_key = gaussian(key_list[3], (3, SLOTS * HEAD_DIM, D), D ** -0.5, 0.125, ((1, 4),))
    w_value = gaussian(key_list[4], (3, SLOTS * HEAD_DIM, D), D ** -0.5, 0.125, ((1, 4),))
    w_out = gaussian(key_list[5], (SLOTS * HEAD_DIM, D), (SLOTS * HEAD_DIM) ** -0.5, 0.25, ((1, 4),))
    return {"tokens": tokens, "norm_gain": norm_gain, "w_query": w_query, "w_key": w_key, "w_value": w_value, "w_out": w_out}


NEG_BIG = -1e+30

def attend(query, context, first_pos, dilation_step, slopes):
    head_count = slopes.shape[0]
    width = query.shape[1] // head_count
    row_count = query.shape[0]
    query_len = row_count // dilation_step
    key_len = context.shape[0] // dilation_step
    query_heads = query.reshape(query_len, dilation_step, head_count, width).transpose(1, 2, 0, 3)
    split_context = context.reshape(key_len, dilation_step, 2, head_count, width)
    key_heads = split_context[:, :, 0].transpose(1, 2, 0, 3)
    value_heads = split_context[:, :, 1].transpose(1, 2, 0, 3)
    scores = jnp.einsum('rhqe,rhke->rhqk', query_heads.astype(jnp.float32), key_heads.astype(jnp.float32)) * (1.0 / math.sqrt(width))
    query_index = jnp.arange(query_len, dtype=jnp.int32)[:, None]
    key_index = jnp.arange(key_len, dtype=jnp.int32)[None, :]
    distance = query_index + STEPS - key_index
    residue = jnp.arange(dilation_step, dtype=jnp.int32)[:, None, None, None]
    key_pos = first_pos - STEPS * dilation_step + key_index[None, None] * dilation_step + residue
    valid = (distance >= 0) & (distance <= STEPS) & (key_pos >= 0)
    logits = scores - slopes[None, :, None, None] * distance.astype(jnp.float32)
    logits = jnp.where(valid, logits, NEG_BIG)
    row_max = lax.optimization_barrier(jnp.max(logits, axis=-1, keepdims=True))
    row_sum = lax.optimization_barrier(jnp.sum(jnp.exp(logits - row_max), axis=-1, keepdims=True))
    log_total = row_max + jnp.log(row_sum)
    weights = jnp.exp(logits - log_total).astype(jnp.bfloat16)
    outputs = jnp.einsum('rhqk,rhke->rhqe', weights.astype(jnp.float32), value_heads.astype(jnp.float32))
    outputs = outputs.transpose(2, 0, 1, 3).reshape(row_count, head_count, width)
    log_total = log_total[..., 0].transpose(2, 0, 1).reshape(row_count, head_count)
    return (outputs, log_total)

def reference(tokens, norm_gain, w_query, w_key, w_value, w_out):
    total_rows = tokens.shape[0]
    scaled = tokens.astype(jnp.float32)
    normed = (scaled * lax.rsqrt(lax.optimization_barrier(jnp.mean(scaled * scaled, axis=-1, keepdims=True)) + 1e-06) * norm_gain).astype(jnp.bfloat16)
    normed_wide = normed.astype(jnp.float32)
    query_rows = jnp.einsum('td,gcd->gtc', normed_wide, w_query.astype(jnp.float32)).astype(jnp.bfloat16)
    keys = jnp.einsum('td,gcd->gtc', normed_wide, w_key.astype(jnp.float32)).astype(jnp.bfloat16)
    value_rows = jnp.einsum('td,gcd->gtc', normed_wide, w_value.astype(jnp.float32)).astype(jnp.bfloat16)
    slot_ids = jnp.arange(SLOTS, dtype=jnp.int32)
    blocks = total_rows // TOK_DEV
    dilation_list = (1, MIDDLE_DILATION, WIDE_DILATION)
    outputs_all = []
    logs_all = []
    for cohort in range(3):
        dilation_step = dilation_list[cohort]
        slopes = jnp.exp2(-8.0 * (cohort * SLOTS + slot_ids + 1).astype(jnp.float32) / (3 * SLOTS))
        key_value = jnp.concatenate([keys[cohort], value_rows[cohort]], axis=-1)
        padded = jnp.concatenate([jnp.zeros((STEPS * dilation_step, key_value.shape[1]), jnp.bfloat16), key_value], axis=0)
        query_all = query_rows[cohort]

        def one_block(block_number):
            start = block_number * TOK_DEV
            query_block = lax.dynamic_slice_in_dim(query_all, start, TOK_DEV, 0)
            context = lax.dynamic_slice_in_dim(padded, start, STEPS * dilation_step + TOK_DEV, 0)
            return attend(query_block, context, start, dilation_step, slopes)
        block_out, block_log = lax.map(one_block, jnp.arange(blocks, dtype=jnp.int32))
        outputs_all.append(block_out.reshape(total_rows, SLOTS, HEAD_DIM))
        logs_all.append(block_log.reshape(total_rows, SLOTS))
    stacked = jnp.stack(logs_all)
    log_weight = jax.nn.logsumexp(stacked, axis=0)
    shares = jnp.exp(stacked - log_weight[None])
    mixture = lax.optimization_barrier(jnp.sum(shares[..., None] * jnp.stack(outputs_all), axis=0))
    mixture = mixture.reshape(total_rows, SLOTS * HEAD_DIM).astype(jnp.bfloat16)
    projected = jnp.dot(mixture, w_out, preferred_element_type=jnp.float32).astype(jnp.bfloat16)
    return (projected, log_weight.T)
```

```python
import functools
import math

import jax
import jax.numpy as jnp
from jax import lax
from jax.experimental import pallas as pl
from jax.experimental.pallas import tpu as pltpu
from jax.sharding import PartitionSpec as P

HEAD_DIM = 64
STEPS = 128
DILATIONS = (1, 4, 16)
NEG_BIG = -1e30
CHUNKS = 2
STORE_LIMIT = 8 * 1024 * 1024
VMEM_LIMIT = 56098816
MESH = pl.DeviceIdType.MESH


def streams_of(dilation, rows):
    count = dilation
    while (rows // count) % 16:
        count //= 2
    return count


def kernel(
    n_sp, n_tp, total_slots, swap,
    tok_hbm, gain_hbm, wq_hbm, wk_hbm, wv_hbm,
    every_ref, logw_ref,
    tok, gain, w_all, normed, acc, qs1, qs2, qs3, ctx1, ctx2, ctx3,
    outs, lses, mix, going, stream, answer, back,
    in_sem, zs, zr, ys, yr, ms, mr, gs, gr, bs, br,
):
    rows, width = tok.shape
    cols = wq_hbm.shape[1]
    heads = cols // HEAD_DIM
    wide = acc.shape[2]
    me = lax.axis_index("sp")
    tp = lax.axis_index("tp")
    even = lax.rem(me, 2) == 0
    odd = lax.rem(me, 2) == 1
    partner = me + 1 - 2 * lax.rem(me, 2)
    ctxs = (ctx1, ctx2, ctx3)
    queries = (qs1, qs2, qs3)

    loads = {}
    def load(name, src, dst):
        loads[name] = pltpu.make_async_copy(src, dst, in_sem.at[len(loads)])
        loads[name].start()
    load("tok", tok_hbm, tok)
    load("gain", gain_hbm, gain)
    load(("q", 2), wq_hbm.at[2], w_all.at[2, 0:cols])
    for g in (2, 0, 1):
        load(("k", g), wk_hbm.at[g], w_all.at[g, cols:2 * cols])
        load(("v", g), wv_hbm.at[g], w_all.at[g, 2 * cols:3 * cols])
    for g in (1, 0):
        load(("q", g), wq_hbm.at[g], w_all.at[g, 0:cols])

    geo = []
    for g, dilation in enumerate(DILATIONS):
        s = ctxs[g].shape[0]
        m = rows // s
        halo = STEPS * dilation // s
        full = ctxs[g].shape[1] - m
        geo.append((s, m, halo, full))

    for g in range(2 if swap else 3):
        s, m, halo, full = geo[g]
        for p in range(s):
            ctxs[g][p, 0:full, :] = jnp.zeros((full, 2 * cols), jnp.bfloat16)

    barrier = pltpu.get_barrier_semaphore()
    if swap:
        for k in range(1, n_sp):
            pl.semaphore_signal(
                barrier, inc=1, device_id={"sp": lax.rem(me + k, n_sp)}, device_id_type=MESH)
    for by in () if swap else (1, 2):
        @pl.when(me >= by)
        def _():
            pl.semaphore_signal(barrier, inc=1, device_id={"sp": me - by}, device_id_type=MESH)
        @pl.when(me + by < n_sp)
        def _():
            pl.semaphore_signal(barrier, inc=1, device_id={"sp": me + by}, device_id_type=MESH)
    for k in range(1, n_tp):
        pl.semaphore_signal(barrier, inc=1, device_id={"tp": lax.rem(tp + k, n_tp)}, device_id_type=MESH)

    loads["tok"].wait()
    loads["gain"].wait()
    part = 32
    @pl.loop(0, rows // part)
    def _(j):
        at = pl.ds(pl.multiple_of(j * part, part), part)
        x = tok[at, :].astype(jnp.float32)
        scale = lax.rsqrt(jnp.mean(x * x, axis=-1, keepdims=True) + 1e-06)
        normed[at, :] = (x * scale * gain[...]).astype(jnp.bfloat16)

    NT = (((1,), (1,)), ((), ()))

    def key_value(g):
        s, m, halo, full = geo[g]
        loads["k", g].wait()
        loads["v", g].wait()
        both = lax.dot_general(
            normed[...], w_all[g, cols:3 * cols, :], NT, preferred_element_type=jnp.float32
        )
        if s == 1:
            ctxs[g][0, full:full + m, :] = both.astype(jnp.bfloat16)
            return
        acc[0, :, 0:cols] = both[:, 0:cols]
        acc[1, :, 0:cols] = both[:, cols:2 * cols]
        for p in range(s):
            for c in range(2):
                piece = acc[c, pl.ds(p, m, stride=s), :]
                ctxs[g][p, full:full + m, c * cols:(c + 1) * cols] = piece[:, 0:cols].astype(jnp.bfloat16)

    def query(g):
        s, m, halo, full = geo[g]
        loads["q", g].wait()
        got = lax.dot_general(
            normed[...], w_all[g, 0:cols, :], NT, preferred_element_type=jnp.float32
        )
        scale = 1.0 / math.sqrt(HEAD_DIM)
        if s == 1:
            queries[g][0] = got.astype(jnp.bfloat16) * jnp.bfloat16(scale)
            return
        acc[0, :, 0:cols] = got
        for p in range(s):
            piece = acc[0, pl.ds(p, m, stride=s), :]
            queries[g][p] = piece[:, 0:cols].astype(jnp.bfloat16) * jnp.bfloat16(scale)

    def region(g, back, streams, last=None):
        s, m, halo, full = geo[g]
        unit = m if g else STEPS
        stop = full - (back - 1) * unit if back else full + m
        size = unit if last is None else last
        return ctxs[g].at[streams, stop - size:stop, :]

    def z_copy(g, src, dst, slot, streams, last=None):
        return pltpu.make_async_remote_copy(
            region(g, src, streams, last), region(g, dst, streams, last),
            zs.at[slot], zr.at[slot], device_id={"sp": me + 2}, device_id_type=MESH)

    def y_copy(g, src, dst, slot, streams):
        return pltpu.make_async_remote_copy(
            region(g, src, streams), region(g, dst, streams),
            ys.at[slot], yr.at[slot], device_id={"sp": partner}, device_id_type=MESH)

    def on(cond, f):
        @pl.when(cond)
        def _():
            f()

    s3 = geo[2][0]
    per = s3 // CHUNKS
    full2 = pl.ds(0, geo[1][0])
    full1 = pl.ds(0, 1)
    tail3 = geo[2][2] - 5 * geo[2][1]
    tail2 = geo[1][2] - geo[1][1]
    z_list = []
    y_list = []
    for k in range(3):
        for c in range(CHUNKS):
            streams = pl.ds(c * per, per)
            z_list.append((2, 2 * k, k * CHUNKS + c, streams, tail3 if k == 2 else None))
            y_list.append((2, 2 * k, k * CHUNKS + c, streams))
    z_list += [(1, 0, 3 * CHUNKS, full2, tail2), (0, 0, 3 * CHUNKS + 1, full1, 0)]
    y_list += [(1, 0, 3 * CHUNKS, full2), (0, 0, 3 * CHUNKS + 1, full1)]

    def z_each(entry, has, act):
        g, src, slot, streams, tail = entry
        if tail is None:
            on(has, lambda: act(z_copy(g, src, src + 2, slot, streams)))
        else:
            if tail:
                on(has & even, lambda: act(z_copy(g, src, src + 2, slot, streams, tail)))
            on(has & odd, lambda: act(z_copy(g, src, src + 2, slot, streams)))

    def z_start(entry):
        z_each(entry, (me >= entry[1]) & (me + 2 < n_sp), lambda c: c.start())

    def z_sent(entry):
        z_each(entry, (me >= entry[1]) & (me + 2 < n_sp), lambda c: c.wait_send())

    def z_recv(entry):
        z_each(entry, me >= entry[1] + 2, lambda c: c.wait_recv())

    def y_even(entry, act):
        g, src, slot, streams = entry
        on(even & (me >= src), lambda: act(y_copy(g, src, src + 1, slot, streams)))

    def y_odd(entry, act):
        g, src, slot, streams = entry
        on(odd & (me >= src + 2), lambda: act(y_copy(g, src + 2, src + 1, slot, streams)))

    def y_recv(entry):
        g, src, slot, streams = entry
        on(me >= src + 1, lambda: y_copy(g, src, src + 1, slot, streams).wait_recv())

    start = lambda c: c.start()
    sent = lambda c: c.wait_send()
    z3 = lambda k: z_list[k * CHUNKS:(k + 1) * CHUNKS]
    y3 = lambda k: y_list[k * CHUNKS:(k + 1) * CHUNKS]

    def whole_stream():
        s, m, halo, full = geo[2]
        for name in "qkv":
            loads[name, 2].wait()
        got = lax.dot_general(normed[...], w_all[2], NT, preferred_element_type=jnp.float32)
        for c in range(3):
            acc[c] = got[:, c * cols:(c + 1) * cols]
        for p in range(s):
            for c in range(3):
                piece = acc[c, pl.ds(p, m, stride=s), :].astype(jnp.bfloat16)
                if c == 0:
                    piece = piece * jnp.bfloat16(1.0 / math.sqrt(HEAD_DIM))
                going[p, :, c * cols:(c + 1) * cols] = piece

    per_dev = geo[2][1]

    def mine_at(e):
        return pl.ds(pl.multiple_of(e * per_dev, 16), per_dev)

    def go(e, source):
        return pltpu.make_async_remote_copy(
            going.at[e], stream.at[mine_at(source), :], gs.at[e], gr.at[source],
            device_id={"sp": e}, device_id_type=MESH)

    def reply(e, source):
        return pltpu.make_async_remote_copy(
            answer.at[e * per_dev:(e + 1) * per_dev, :], back.at[source], bs.at[e], br.at[source],
            device_id={"sp": e}, device_id_type=MESH)

    def go_arrival(source):
        pltpu.make_async_remote_copy(
            going.at[source], stream.at[mine_at(source), :], gs.at[source], gr.at[source],
            device_id={"sp": source}, device_id_type=MESH).wait_recv()

    def reply_arrival(source):
        pltpu.make_async_remote_copy(
            answer.at[source * per_dev:(source + 1) * per_dev, :], back.at[source],
            bs.at[source], br.at[source],
            device_id={"sp": source}, device_id_type=MESH).wait_recv()

    def each_peer(f, peers=None):
        for e in peers or range(n_sp):
            on(me != e, lambda: f(e))

    if swap:
        whole_stream()
    else:
        key_value(2)
    if swap:
        peers = n_sp - 1 + n_tp - 1
    else:
        peers = jnp.minimum(me, 2) + jnp.minimum(n_sp - 1 - me, 2) + (n_tp - 1)
    pl.semaphore_wait(barrier, peers)
    if swap:
        each_peer(lambda e: go(e, me).start())
        stream[mine_at(me), :] = going[me]
    else:
        for c in range(CHUNKS):
            z_start(z3(0)[c])
            y_even(y3(0)[c], start)
    def near(entry):
        g, by, slot, last = entry
        streams = full2 if g else full1
        return pltpu.make_async_remote_copy(
            region(g, 0, streams, last), region(g, by, streams, last),
            zs.at[slot], zr.at[slot], device_id={"sp": me + by}, device_id_type=MESH)

    def near_start(entry):
        on(me + entry[1] < n_sp, lambda: near(entry).start())

    def near_sent(entry):
        on(me + entry[1] < n_sp, lambda: near(entry).wait_send())

    def near_recv(entry):
        on(me >= entry[1], lambda: near(entry).wait_recv())

    near_list = [(0, 1, 0, None), (1, 1, 1, None), (1, 2, 2, tail2)]
    if swap:
        key_value(0)
        near_start(near_list[0])
        key_value(1)
        near_start(near_list[1])
        near_start(near_list[2])
    else:
        key_value(1)
        z_start(z_list[-2])
        y_even(y_list[-2], start)
        key_value(0)
        z_start(z_list[-1])
        y_even(y_list[-1], start)
    for g in (0, 1) if swap else (0, 1, 2):
        query(g)

    def relay(k):
        for c in range(CHUNKS):
            z_recv(z3(k - 1)[c])
            z_start(z3(k)[c])
            y_odd(y3(k - 1)[c], start)
            y_even(y3(k)[c], start)

    lane_head = lax.broadcasted_iota(jnp.int32, (1, cols), 1) // HEAD_DIM

    def bias_of(g, height, length, first_key, offset):
        s = geo[g][0]
        halo = geo[g][2]
        ratio = DILATIONS[g] // s
        row = lax.broadcasted_iota(jnp.int32, (height, length), 0)
        col = lax.broadcasted_iota(jnp.int32, (height, length), 1)
        apart = row + offset - col
        step = apart // ratio
        valid = (apart >= 0) & (apart <= STEPS * ratio)
        if ratio > 1:
            valid = valid & (apart % ratio == 0)
        valid = valid & ((col + first_key) * s >= halo * s - me * rows)
        parts = []
        for h in range(heads):
            slot = (g * total_slots + tp * heads + h + 1).astype(jnp.float32)
            slope = jnp.exp2(jnp.full((1, 1), -8.0 / (3 * total_slots), jnp.float32) * slot)
            parts.append(jnp.where(valid, -slope * step.astype(jnp.float32), NEG_BIG))
        return jnp.concatenate(parts, axis=0) if heads > 1 else parts[0]

    def attend(q, keys, values, bias):
        height = q.shape[0]
        stacked = [jnp.where(lane_head == h, q, jnp.zeros_like(q)) for h in range(heads)]
        stacked = jnp.concatenate(stacked, axis=0) if heads > 1 else stacked[0]
        logits = lax.dot_general(stacked, keys, NT, preferred_element_type=jnp.float32) + bias
        top = jnp.max(logits, axis=-1, keepdims=True)
        e = jnp.exp(logits - top)
        total = jnp.sum(e, axis=-1, keepdims=True)
        lse = top + jnp.log(total)
        weights = (e * (1.0 / total)).astype(jnp.bfloat16)
        o = jnp.dot(weights, values, preferred_element_type=jnp.float32)
        out = o[0:height]
        log = jnp.broadcast_to(lse[0:height], (height, cols))
        for h in range(1, heads):
            mine = lane_head == h
            out = jnp.where(mine, o[h * height:(h + 1) * height], out)
            log = jnp.where(mine, lse[h * height:(h + 1) * height], log)
        return out, log

    def put(g, at, out, log):
        if cols < wide:
            out = jnp.concatenate([out] * (wide // cols), axis=1)
            log = jnp.concatenate([log] * (wide // cols), axis=1)
        outs[g, at, :] = out
        lses[g, at, :] = log

    def attend_group(g, first, count):
        s, m, halo, full = geo[g]
        base = full - halo
        bias = bias_of(g, m, halo + m, 0, halo)
        for p in range(first, first + count):
            out, log = attend(
                queries[g][p], ctxs[g][p, base:full + m, 0:cols],
                ctxs[g][p, base:full + m, cols:2 * cols], bias)
            put(g, pl.ds(p, m, stride=s), out, log)

    tile = STEPS

    def near_tile(j):
        base = geo[0][3] - STEPS + j * tile
        bias = bias_of(0, tile, tile + STEPS, j * tile, STEPS)
        out, log = attend(
            qs1[0, j * tile:(j + 1) * tile, :], ctx1[0, base:base + tile + STEPS, 0:cols],
            ctx1[0, base:base + tile + STEPS, cols:2 * cols], bias)
        put(0, pl.ds(j * tile, tile), out, log)

    def pass_on(entry, y_entry):
        z_recv(entry)
        y_odd(y_entry, start)

    same_head = (
        lax.broadcasted_iota(jnp.int32, (cols, cols), 0) // HEAD_DIM
        == lax.broadcasted_iota(jnp.int32, (cols, cols), 1) // HEAD_DIM
    ).astype(jnp.bfloat16)

    def stream_tile(j):
        stop = (j + 1) * tile
        s = geo[2][0]
        ratio = DILATIONS[2] // s
        row = lax.broadcasted_iota(jnp.int32, (tile, stop), 0)
        col = lax.broadcasted_iota(jnp.int32, (tile, stop), 1)
        apart = row + j * tile - col
        valid = (apart >= 0) & (apart <= STEPS * ratio) & (apart % ratio == 0)
        parts = []
        for h in range(heads):
            slot = (2 * total_slots + tp * heads + h + 1).astype(jnp.float32)
            slope = jnp.exp2(jnp.full((1, 1), -8.0 / (3 * total_slots), jnp.float32) * slot)
            parts.append(jnp.where(valid, -slope * (apart // ratio).astype(jnp.float32), NEG_BIG))
        bias = jnp.concatenate(parts, axis=0) if heads > 1 else parts[0]
        out, log = attend(
            stream[j * tile:stop, 0:cols], stream[0:stop, cols:2 * cols],
            stream[0:stop, 2 * cols:3 * cols], bias)
        high = log.astype(jnp.bfloat16).astype(jnp.float32)
        mid = (log - high).astype(jnp.bfloat16).astype(jnp.float32)
        low = log - high - mid
        place = lax.rem(lax.broadcasted_iota(jnp.int32, (1, cols), 1), HEAD_DIM)
        terms = jnp.where(place == 0, high, jnp.where(place == 1, mid, jnp.where(place == 2, low, 0.0)))
        answer[j * tile:stop, 0:cols] = out.astype(jnp.bfloat16)
        answer[j * tile:stop, cols:2 * cols] = terms.astype(jnp.bfloat16)

    if swap:
        for j in range(1, rows // tile):
            near_tile(j)
        each_peer(lambda e: go_arrival(e))
        done = 0
        for j in range(rows // tile):
            stream_tile(j)
            ready = (j + 1) * tile // per_dev
            each_peer(lambda e: reply(e, me).start(), range(done, ready))
            done = ready
        back[me] = answer[mine_at(me), :]
        near_recv(near_list[0])
        near_tile(0)
        near_recv(near_list[1])
        near_recv(near_list[2])
        attend_group(1, 0, geo[1][0])
        each_peer(lambda e: reply_arrival(e))
        for e in range(n_sp):
            log = jnp.dot(back[e, :, cols:2 * cols], same_head, preferred_element_type=jnp.float32)
            put(2, pl.ds(e, per_dev, stride=n_sp), back[e, :, 0:cols].astype(jnp.float32), log)
    else:
        relay(1)
        pass_on(z_list[-2], y_list[-2])
        pass_on(z_list[-1], y_list[-1])
        y_recv(y_list[-1])
        for j in range(rows // tile):
            near_tile(j)
        relay(2)
        y_recv(y_list[-2])
        attend_group(1, 0, geo[1][0])
        for c in range(CHUNKS):
            pass_on(z3(2)[c], y3(2)[c])
        for c in range(CHUNKS):
            for k in range(3):
                y_recv(y3(k)[c])
            attend_group(2, c * per, per)

    for j in range(rows // tile):
        at = pl.ds(j * tile, tile)
        logs = [lses[g, at, :] for g in range(3)]
        top = jnp.maximum(jnp.maximum(logs[0], logs[1]), logs[2])
        lw = top + jnp.log(sum(jnp.exp(l - top) for l in logs))
        mixed = sum(jnp.exp(logs[g] - lw) * outs[g, at, :] for g in range(3))
        mix[tp, at, :] = mixed[:, 0:cols].astype(jnp.bfloat16)
        flipped = lw.T
        for h in range(heads):
            logw_ref[h:h + 1, j * tile:(j + 1) * tile] = flipped[h * HEAD_DIM:h * HEAD_DIM + 1, :]

    def spread(k):
        to = lax.rem(tp + k, n_tp)
        return pltpu.make_async_remote_copy(
            mix.at[tp], mix.at[tp], ms.at[k - 1], mr.at[k - 1],
            device_id={"tp": to}, device_id_type=MESH)

    def arrival(k):
        source = lax.rem(tp + n_tp - k, n_tp)
        return pltpu.make_async_remote_copy(
            mix.at[source], mix.at[source], ms.at[k - 1], mr.at[k - 1],
            device_id={"tp": lax.rem(tp + k, n_tp)}, device_id_type=MESH)

    for k in range(1, n_tp):
        spread(k).start()
    for k in range(1, n_tp):
        arrival(k).wait_recv()
    for t in range(n_tp):
        every_ref[:, t * cols:(t + 1) * cols] = mix[t]

    for k in range(1, n_tp):
        spread(k).wait_send()
    if swap:
        each_peer(lambda e: go(e, me).wait_send())
        each_peer(lambda e: reply(e, me).wait_send())
        for entry in near_list:
            near_sent(entry)
    for entry in () if swap else z_list:
        z_sent(entry)
    for entry in () if swap else y_list:
        y_even(entry, sent)
        y_odd(entry, sent)


LANES = 128
NT = (((1,), (1,)), ((), ()))


def split_kernel(
    n_sp, n_tp, total_slots,
    tok_hbm, gain_hbm, wq_hbm, wk_hbm, wv_hbm, wo_hbm,
    proj_ref, logw_ref,
    tok, gain, w_all, w_out, normed, acc, q1, q2, ctx1, ctx2, going, stream, qfar,
    answer, answer_far, lse_near, lse_far, back, back_far, back_lse, back_far_lse,
    b0, b0_first, b1, b2, b3, out0, log0, part_o, part_l, mix, nat, lw_nat,
    in_sem, gs, gr, fs, fr, ns, nr, as_, ar, ls, lr, bs, br, cs, cr, ms, mr,
):
    rows, width = tok.shape
    cols = wq_hbm.shape[1]
    heads = cols // HEAD_DIM
    classes = going.shape[0]
    per = rows // classes
    ratio = DILATIONS[2] // classes
    tile = STEPS
    me = lax.axis_index("sp")
    tp = lax.axis_index("tp")
    mine = lax.rem(me, classes)
    base = me - mine
    upper = me >= classes
    lower = me < classes

    loads = {}

    def load(name, src, dst):
        loads[name] = pltpu.make_async_copy(src, dst, in_sem.at[len(loads)])
        loads[name].start()

    for c in range(classes):
        at = pl.ds(c * per, per)
        load(("tok", c), tok_hbm.at[at], tok.at[at])
        if c == 0:
            load("gain", gain_hbm, gain)
    slot = 0
    weights = (
        (2, "q"), (2, "k"), (2, "v"), (1, "k"), (1, "v"), (0, "k"), (0, "v"), (1, "q"), (0, "q"))
    for g, kind in weights:
        src = {"q": wq_hbm, "k": wk_hbm, "v": wv_hbm}[kind]
        load((kind, g), src.at[g], w_all.at[slot * cols:(slot + 1) * cols])
        slot += 1
    load("out", wo_hbm, w_out)

    barrier = pltpu.get_barrier_semaphore()
    for k in range(1, n_sp):
        pl.semaphore_signal(
            barrier, inc=1, device_id={"sp": lax.rem(me + k, n_sp)}, device_id_type=MESH)
    for k in range(1, n_tp):
        pl.semaphore_signal(
            barrier, inc=1, device_id={"tp": lax.rem(tp + k, n_tp)}, device_id_type=MESH)

    @pl.when(me == 0)
    def _():
        ctx1[0:tile, :] = jnp.zeros((tile, 2 * cols), jnp.bfloat16)
        for p in range(classes):
            ctx2[p, 0:tile, :] = jnp.zeros((tile, 2 * cols), jnp.bfloat16)

    @pl.when(me == 1)
    def _():
        for p in range(classes):
            ctx2[p, 0:tile - per, :] = jnp.zeros((tile - per, 2 * cols), jnp.bfloat16)

    def bias(g, height, first, last, offset, step, key_limit):
        row = lax.broadcasted_iota(jnp.int32, (height, last - first), 0)
        col = lax.broadcasted_iota(jnp.int32, (height, last - first), 1) + first
        apart = row + offset - col
        valid = (apart >= 0) & (apart <= STEPS * step)
        shift = step.bit_length() - 1
        if step > 1:
            valid = valid & ((apart & (step - 1)) == 0)
        if key_limit is not None:
            valid = valid & (col >= key_limit)
        far = lax.shift_right_arithmetic(apart, shift).astype(jnp.float32)
        parts = []
        for h in range(heads):
            slot = (g * total_slots + tp * heads + h + 1).astype(jnp.float32)
            slope = jnp.exp2(jnp.full((1, 1), -8.0 / (3 * total_slots), jnp.float32) * slot)
            parts.append(jnp.where(valid, -slope * far, NEG_BIG))
        return parts

    def keep(ref, parts):
        height, length = parts[0].shape
        for h in range(heads):
            ref[h * height:(h + 1) * height, 0:length] = parts[h]

    def near_keys(k):
        return -(-(k + 1) * per // LANES) * LANES

    def far_keys(k):
        return max(0, (rows + k * per - STEPS * ratio) // LANES * LANES)

    keep(b0, bias(0, tile, 0, 2 * tile, tile, 1, None))
    keep(b0_first, bias(0, tile, 0, 2 * tile, tile, 1, jnp.where(me == 0, tile, 0)))
    keep(b1, bias(1, per, 0, tile + per, tile, 1, jnp.maximum(tile - me * per, 0)))
    for k in range(classes):
        keep(b2.at[k], bias(2, per, 0, near_keys(k), k * per, ratio, None))
        keep(b3.at[k], bias(2, per, far_keys(k), rows, rows + k * per, ratio, None))

    loads["gain"].wait()
    part = 32
    for c in range(classes):
        loads["tok", c].wait()
        for j in range(per // part):
            at = pl.ds(c * per + j * part, part)
            x = tok[at, :].astype(jnp.float32)
            scale = lax.rsqrt(jnp.mean(x * x, axis=-1, keepdims=True) + 1e-06)
            normed[at, :] = (x * scale * gain[...]).astype(jnp.bfloat16)

    def product(first, count):
        for g, kind in weights[first:first + count]:
            loads[kind, g].wait()
        return lax.dot_general(
            normed[...], w_all[first * cols:(first + count) * cols, :], NT,
            preferred_element_type=jnp.float32)

    def by_class(n, p):
        return acc[n, pl.ds(p, per, stride=classes), :].astype(jnp.bfloat16)

    scaling = jnp.bfloat16(1.0 / math.sqrt(HEAD_DIM))
    got = product(0, 3)
    for n in range(3):
        acc[n] = got[:, n * cols:(n + 1) * cols]
    for p in range(classes):
        going[p, :, 0:cols] = by_class(0, p) * scaling
        going[p, :, cols:2 * cols] = by_class(1, p)
        going[p, :, 2 * cols:3 * cols] = by_class(2, p)

    def slice_of(k):
        return pl.ds(pl.multiple_of(k * per, 16), per)

    def remote(src, dst, send, recv, sp):
        return pltpu.make_async_remote_copy(
            src, dst, send, recv, device_id={"sp": sp}, device_id_type=MESH)

    def go(c, source):
        return remote(going.at[c], stream.at[slice_of(source), :], gs.at[c], gr.at[source], base + c)

    def go_far(c, source):
        return remote(going.at[c, :, 0:cols], qfar.at[source], fs.at[c], fr.at[source], c)

    def reply(e, source):
        return remote(answer.at[e], back.at[source], as_.at[e], ar.at[source], base + e)

    def reply_lse(e, source):
        return remote(lse_near.at[e], back_lse.at[source], ls.at[e], lr.at[source], base + e)

    def reply_far(e, source):
        return remote(
            answer_far.at[e], back_far.at[source], bs.at[e], br.at[source], classes + e)

    def reply_far_lse(e, source):
        return remote(
            lse_far.at[e], back_far_lse.at[source], cs.at[e], cr.at[source], classes + e)

    def when(cond, f):
        @pl.when(cond)
        def _():
            f()

    def each_peer(f):
        for e in range(classes):
            when(mine != e, lambda: f(e))

    tail = tile - per
    full2 = pl.ds(0, classes)

    def near(n):
        if n == 0:
            src, dst, by = ctx1.at[rows:rows + tile, :], ctx1.at[0:tile, :], 1
        elif n == 1:
            src, dst, by = ctx2.at[full2, tile:tile + per, :], ctx2.at[full2, tail:tile, :], 1
        else:
            src, dst, by = ctx2.at[full2, tile + per - tail:tile + per, :], ctx2.at[full2, 0:tail, :], 2
        return by, remote(src, dst, ns.at[n], nr.at[n], me + by)

    def near_start(n):
        by, copy = near(n)
        when(me + by < n_sp, copy.start)

    def near_sent(n):
        by, copy = near(n)
        when(me + by < n_sp, copy.wait_send)

    def near_arrival(n):
        by, copy = near(n)
        when(me >= by, copy.wait_recv)

    pl.semaphore_wait(barrier, n_sp - 1 + n_tp - 1)

    @pl.when(upper)
    def _():
        for c in range(classes):
            go_far(c, mine).start()

    each_peer(lambda e: go(e, mine).start())
    stream[slice_of(mine), :] = going[mine]

    got = product(3, 4)
    for n in range(2):
        acc[n] = got[:, n * cols:(n + 1) * cols]
    for p in range(classes):
        for n in range(2):
            ctx2[p, tile:tile + per, n * cols:(n + 1) * cols] = by_class(n, p)
    ctx1[tile:tile + rows, :] = got[:, 2 * cols:4 * cols].astype(jnp.bfloat16)

    got = product(7, 2)
    acc[2] = got[:, 0:cols]
    for p in range(classes):
        q2[p] = by_class(2, p) * scaling
    q1[...] = got[:, cols:2 * cols].astype(jnp.bfloat16) * scaling

    lane = lax.broadcasted_iota(jnp.int32, (1, cols), 1)
    lane_head = lane // HEAD_DIM
    lane_turn = lax.rem(lane, heads)

    def attend(q, keys, values, bias_ref, length):
        height = q.shape[0]
        stacked = jnp.concatenate(
            [jnp.where(lane_head == h, q, jnp.zeros_like(q)) for h in range(heads)], axis=0)
        logits = lax.dot_general(stacked, keys, NT, preferred_element_type=jnp.float32)
        logits = logits + bias_ref[0:heads * height, 0:length]
        top = jnp.max(logits, axis=-1, keepdims=True)
        e = jnp.exp(logits - top)
        total = jnp.sum(e, axis=-1, keepdims=True)
        o = jnp.dot(e.astype(jnp.bfloat16), values, preferred_element_type=jnp.float32)
        o = o * (1.0 / total)
        lse = top + jnp.log(total)
        out = o[0:height]
        for h in range(1, heads):
            out = jnp.where(lane_head == h, o[h * height:(h + 1) * height], out)
        return out, [lse[h * height:(h + 1) * height] for h in range(heads)]

    def lanes_of(lse, pattern):
        log = jnp.broadcast_to(lse[0], (lse[0].shape[0], cols))
        for h in range(1, heads):
            log = jnp.where(pattern == h, lse[h], log)
        return log

    def pack(ref, k, lse):
        ref[k, :, 0:per] = lanes_of(lse, lane_turn).T[0:heads, :]

    def unpack(ref, k):
        row = ref[k]
        wide = [jnp.broadcast_to(row[h:h + 1, :], (HEAD_DIM, LANES)) for h in range(heads)]
        return jnp.concatenate(wide, axis=0).T[0:per, :]

    def near_tile(j, bias_ref):
        first = j * tile
        out, lse = attend(
            q1[first:first + tile, :], ctx1[first:first + 2 * tile, 0:cols],
            ctx1[first:first + 2 * tile, cols:2 * cols], bias_ref, 2 * tile)
        out0[first:first + tile, :] = out
        log0[first:first + tile, :] = lanes_of(lse, lane_head)

    for j in range(1, rows // tile):
        near_tile(j, b0)
    near_start(1)
    near_start(2)
    near_start(0)

    def go_arrival(k):
        go(k, k).wait_recv()

    each_peer(go_arrival)
    for k in range(classes):
        stop = near_keys(k)
        out, lse = attend(
            stream[k * per:(k + 1) * per, 0:cols], stream[0:stop, cols:2 * cols],
            stream[0:stop, 2 * cols:3 * cols], b2.at[k], stop)
        answer[k] = out.astype(jnp.bfloat16)
        pack(lse_near, k, lse)
    each_peer(lambda e: (reply(e, mine).start(), reply_lse(e, mine).start()))
    back[mine] = answer[mine]
    back_lse[mine] = lse_near[mine]

    @pl.when(lower)
    def _():
        for k in range(classes):
            go_far(k, k).wait_recv()
        for k in range(classes):
            first = far_keys(k)
            out, lse = attend(
                qfar[k], stream[first:rows, cols:2 * cols],
                stream[first:rows, 2 * cols:3 * cols], b3.at[k], rows - first)
            answer_far[k] = out.astype(jnp.bfloat16)
            pack(lse_far, k, lse)
        for k in range(classes):
            reply_far(k, mine).start()
            reply_far_lse(k, mine).start()

    near_arrival(0)
    near_tile(0, b0_first)
    near_arrival(1)
    near_arrival(2)
    near_parts = []
    for p in range(classes):
        near_parts.append(attend(
            q2[p], ctx2[p, :, 0:cols], ctx2[p, :, cols:2 * cols], b1, tile + per))
    for p in range(classes):
        out, lse = near_parts[p]
        part_o[p] = out
        part_l[p] = lanes_of(lse, lane_head)

    def merge(logs, outs):
        top = functools.reduce(jnp.maximum, logs)
        log = top + jnp.log(sum(jnp.exp(l - top) for l in logs))
        return log, sum(jnp.exp(l - log) * o for l, o in zip(logs, outs))

    each_peer(lambda e: (reply(e, e).wait_recv(), reply_lse(e, e).wait_recv()))
    for p in range(classes):
        at = pl.ds(p, per, stride=classes)
        log, out = merge(
            [log0[at, :], part_l[p], unpack(back_lse, p)],
            [out0[at, :], part_o[p], back[p].astype(jnp.float32)])
        part_l[p] = log
        part_o[p] = out

    def spread(k, c):
        return pltpu.make_async_remote_copy(
            mix.at[tp, c], mix.at[tp, c], ms.at[k - 1, c], mr.at[k - 1, c],
            device_id={"tp": lax.rem(tp + k, n_tp)}, device_id_type=MESH)

    def spread_arrival(k, c):
        source = lax.rem(tp + n_tp - k, n_tp)
        return pltpu.make_async_remote_copy(
            mix.at[source, c], mix.at[source, c], ms.at[k - 1, c], mr.at[k - 1, c],
            device_id={"tp": lax.rem(tp + k, n_tp)}, device_id_type=MESH)

    def finish(c):
        @pl.when(upper)
        def _():
            reply_far(c, c).wait_recv()
            reply_far_lse(c, c).wait_recv()
            log, out = merge(
                [part_l[c], unpack(back_far_lse, c)],
                [part_o[c], back_far[c].astype(jnp.float32)])
            part_l[c] = log
            part_o[c] = out

        mix[tp, c] = part_o[c].astype(jnp.bfloat16)
        lw_nat[pl.ds(c, per, stride=classes), :] = part_l[c]
        for k in range(1, n_tp):
            spread(k, c).start()

    def project_class(c):
        for k in range(1, n_tp):
            spread_arrival(k, c).wait_recv()
        mixed = jnp.concatenate([mix[t, c] for t in range(n_tp)], axis=1)
        got = jnp.dot(mixed, w_out[...], preferred_element_type=jnp.float32)
        for n in range(nat.shape[0]):
            nat[n, pl.ds(c, per, stride=classes), :] = got[:, n * LANES:(n + 1) * LANES]

    finish(0)
    finish(1)
    loads["out"].wait()
    for c in range(classes):
        if c + 2 < classes:
            finish(c + 2)
        project_class(c)
    for n in range(nat.shape[0]):
        proj_ref[:, n * LANES:(n + 1) * LANES] = nat[n].astype(jnp.bfloat16)
    for j in range(rows // tile):
        flipped = lw_nat[j * tile:(j + 1) * tile, :].T
        for h in range(heads):
            logw_ref[h:h + 1, j * tile:(j + 1) * tile] = flipped[h * HEAD_DIM:h * HEAD_DIM + 1, :]

    for c in range(classes):
        for k in range(1, n_tp):
            spread(k, c).wait_send()
    each_peer(lambda e: (
        go(e, mine).wait_send(), reply(e, mine).wait_send(), reply_lse(e, mine).wait_send()))

    @pl.when(upper)
    def _():
        for c in range(classes):
            go_far(c, mine).wait_send()

    @pl.when(lower)
    def _():
        for c in range(classes):
            reply_far(c, mine).wait_send()
            reply_far_lse(c, mine).wait_send()

    for n in range(3):
        near_sent(n)


def store(proj_ref, logw_ref, proj_out, logw_out, sem):
    copies = [
        pltpu.make_async_copy(proj_ref, proj_out, sem.at[0]),
        pltpu.make_async_copy(logw_ref, logw_out, sem.at[1]),
    ]
    for copy in copies:
        copy.start()
    for copy in copies:
        copy.wait()


def split_call(n_sp, n_tp, tokens, norm_gain, w_query, w_key, w_value, w_out):
    rows, width = tokens.shape
    cols = w_query.shape[1]
    out_cols = w_out.shape[1]
    heads = cols // HEAD_DIM
    classes = n_sp // 2
    per = rows // classes
    bf, f32 = jnp.bfloat16, jnp.float32
    vmem = pltpu.VMEM
    dma = pltpu.SemaphoreType.DMA
    lanes2 = heads * per
    shapes = (
        jax.ShapeDtypeStruct((rows, out_cols), bf),
        jax.ShapeDtypeStruct((heads, rows), f32),
    )
    results = pl.pallas_call(
        functools.partial(split_kernel, n_sp, n_tp, heads * n_tp),
        out_shape=shapes,
        in_specs=[pl.BlockSpec(memory_space=pltpu.HBM)] * 6,
        out_specs=(pl.BlockSpec(memory_space=pltpu.VMEM),) * 2,
        scratch_shapes=[
            vmem((rows, width), bf),
            vmem((1, width), f32),
            vmem((9 * cols, width), bf),
            vmem(w_out.shape, bf),
            vmem((rows, width), bf),
            vmem((3, rows, cols), f32),
            vmem((rows, cols), bf),
            vmem((classes, per, cols), bf),
            vmem((STEPS + rows, 2 * cols), bf),
            vmem((classes, STEPS + per, 2 * cols), bf),
            vmem((classes, per, 3 * cols), bf),
            vmem((rows, 3 * cols), bf),
            vmem((classes, per, cols), bf),
            vmem((classes, per, cols), bf),
            vmem((classes, per, cols), bf),
            vmem((classes, heads, LANES), f32),
            vmem((classes, heads, LANES), f32),
            vmem((classes, per, cols), bf),
            vmem((classes, per, cols), bf),
            vmem((classes, heads, LANES), f32),
            vmem((classes, heads, LANES), f32),
            vmem((heads * STEPS, 2 * STEPS), f32),
            vmem((heads * STEPS, 2 * STEPS), f32),
            vmem((lanes2, STEPS + per), f32),
            vmem((classes, lanes2, rows), f32),
            vmem((classes, lanes2, rows), f32),
            vmem((rows, cols), f32),
            vmem((rows, cols), f32),
            vmem((classes, per, cols), f32),
            vmem((classes, per, cols), f32),
            vmem((n_tp, classes, per, cols), bf),
            vmem((out_cols // LANES, rows, LANES), f32),
            vmem((rows, cols), f32),
            dma((11 + classes,)),
            dma((classes,)), dma((classes,)), dma((classes,)), dma((classes,)),
            dma((3,)), dma((3,)),
            dma((classes,)), dma((classes,)), dma((classes,)), dma((classes,)),
            dma((classes,)), dma((classes,)), dma((classes,)), dma((classes,)),
            dma((n_tp - 1, classes)), dma((n_tp - 1, classes)),
        ],
        compiler_params=pltpu.CompilerParams(
            collective_id=0, has_side_effects=True, vmem_limit_bytes=VMEM_LIMIT
        ),
    )(tokens, norm_gain.reshape(1, width), w_query, w_key, w_value, w_out)
    return pl.pallas_call(
        store,
        out_shape=shapes,
        in_specs=[pl.BlockSpec(memory_space=pltpu.VMEM)] * 2,
        out_specs=(pl.BlockSpec(memory_space=pl.ANY),) * 2,
        scratch_shapes=[pltpu.SemaphoreType.DMA((2,))],
        compiler_params=pltpu.CompilerParams(vmem_limit_bytes=STORE_LIMIT),
    )(*results)


def splits(n_sp, n_tp, rows, cols, out_cols):
    classes = n_sp // 2
    if n_sp % 2 or classes != DILATIONS[1] or DILATIONS[2] % classes:
        return False
    if cols != LANES or LANES % HEAD_DIM or rows % (classes * 32) or rows % STEPS or out_cols % LANES:
        return False
    per = rows // classes
    window = STEPS * DILATIONS[2] // classes
    return per <= STEPS <= 2 * per and classes * per <= window


def project(every_ref, w_ref, log_ref, proj_ref, logw_ref):
    proj_ref[...] = jnp.dot(
        every_ref[...], w_ref[...], preferred_element_type=jnp.float32
    ).astype(jnp.bfloat16)
    logw_ref[...] = log_ref[...]


def solution(mesh):
    n_sp, n_tp = mesh.shape["sp"], mesh.shape["tp"]

    def per_device(tokens, norm_gain, w_query, w_key, w_value, w_out):
        rows, width = tokens.shape
        cols = w_query.shape[1]
        out_cols = w_out.shape[1]
        heads = cols // HEAD_DIM
        wide = max(cols, 128)
        if splits(n_sp, n_tp, rows, cols, out_cols):
            return split_call(n_sp, n_tp, tokens, norm_gain, w_query, w_key, w_value, w_out)
        bf, f32 = jnp.bfloat16, jnp.float32
        counts = [streams_of(d, rows) for d in DILATIONS]
        m = [rows // s for s in counts]
        slots = 3 * CHUNKS + 2
        swap = n_sp == counts[2] and cols % 128 == 0
        vmem = pltpu.VMEM
        dma = pltpu.SemaphoreType.DMA
        mixed, logs = pl.pallas_call(
            functools.partial(kernel, n_sp, n_tp, heads * n_tp, swap),
            out_shape=(
                jax.ShapeDtypeStruct((rows, n_tp * cols), bf),
                jax.ShapeDtypeStruct((heads, rows), f32),
            ),
            in_specs=[pl.BlockSpec(memory_space=pl.ANY)] * 5,
            out_specs=(pl.BlockSpec(memory_space=pltpu.VMEM),) * 2,
            scratch_shapes=[
                vmem((rows, width), bf),
                vmem((1, width), f32),
                vmem((3, 3 * cols, width), bf),
                vmem((rows, width), bf),
                vmem((3, rows, wide), f32),
                vmem((counts[0], m[0], cols), bf),
                vmem((counts[1], m[1], cols), bf),
                vmem((counts[2], m[2], cols), bf),
                vmem((1, 2 * STEPS + rows, 2 * cols), bf),
                vmem((counts[1], 3 * m[1], 2 * cols), bf),
                vmem((counts[2], 7 * m[2], 2 * cols), bf),
                vmem((3, rows, wide), f32),
                vmem((3, rows, wide), f32),
                vmem((n_tp, rows, cols), bf),
                vmem((counts[2], m[2], 3 * cols), bf),
                vmem((rows, 3 * cols), bf),
                vmem((rows, 2 * cols), bf),
                vmem((counts[2], m[2], 2 * cols), bf),
                dma((12,)),
                dma((slots,)), dma((slots,)), dma((slots,)), dma((slots,)),
                dma((n_tp - 1,)), dma((n_tp - 1,)),
                dma((n_sp,)), dma((n_sp,)), dma((n_sp,)), dma((n_sp,)),
            ],
            compiler_params=pltpu.CompilerParams(
                collective_id=0, has_side_effects=True, vmem_limit_bytes=60 * 1024 * 1024
            ),
        )(tokens, norm_gain.reshape(1, width), w_query, w_key, w_value)
        return pl.pallas_call(
            project,
            out_shape=(
                jax.ShapeDtypeStruct((rows, out_cols), bf),
                jax.ShapeDtypeStruct((heads, rows), f32),
            ),
        )(mixed, w_out, logs)

    in_specs = (
        P("sp", None),
        P(),
        P(None, "tp", None),
        P(None, "tp", None),
        P(None, "tp", None),
        P(None, "tp"),
    )
    out_specs = (P("sp", "tp"), P("tp", "sp"))
    return jax.shard_map(
        per_device, mesh=mesh, in_specs=in_specs, out_specs=out_specs, check_vma=False
    )
```

```python
import functools
import math

import jax
import jax.numpy as jnp
from jax import lax
from jax.experimental import pallas as pl
from jax.experimental.pallas import tpu as pltpu
from jax.sharding import PartitionSpec as P

HEAD_DIM = 64
STEPS = 128
DILATIONS = (1, 4, 16)
NEG_BIG = -1e30
CHUNKS = 2
STORE_LIMIT = 8 * 1024 * 1024
VMEM_LIMIT = 60 * 1024 * 1024
MESH = pl.DeviceIdType.MESH


def streams_of(dilation, rows):
    count = dilation
    while (rows // count) % 16:
        count //= 2
    return count


def kernel(
    n_sp, n_tp, total_slots, swap,
    tok_hbm, gain_hbm, wq_hbm, wk_hbm, wv_hbm,
    every_ref, logw_ref,
    tok, gain, w_all, normed, acc, qs1, qs2, qs3, ctx1, ctx2, ctx3,
    outs, lses, mix, going, stream, answer, back,
    in_sem, zs, zr, ys, yr, ms, mr, gs, gr, bs, br,
):
    rows, width = tok.shape
    cols = wq_hbm.shape[1]
    heads = cols // HEAD_DIM
    wide = acc.shape[2]
    me = lax.axis_index("sp")
    tp = lax.axis_index("tp")
    even = lax.rem(me, 2) == 0
    odd = lax.rem(me, 2) == 1
    partner = me + 1 - 2 * lax.rem(me, 2)
    ctxs = (ctx1, ctx2, ctx3)
    queries = (qs1, qs2, qs3)

    loads = {}
    def load(name, src, dst):
        loads[name] = pltpu.make_async_copy(src, dst, in_sem.at[len(loads)])
        loads[name].start()
    load("tok", tok_hbm, tok)
    load("gain", gain_hbm, gain)
    load(("q", 2), wq_hbm.at[2], w_all.at[2, 0:cols])
    for g in (2, 0, 1):
        load(("k", g), wk_hbm.at[g], w_all.at[g, cols:2 * cols])
        load(("v", g), wv_hbm.at[g], w_all.at[g, 2 * cols:3 * cols])
    for g in (1, 0):
        load(("q", g), wq_hbm.at[g], w_all.at[g, 0:cols])

    geo = []
    for g, dilation in enumerate(DILATIONS):
        s = ctxs[g].shape[0]
        m = rows // s
        halo = STEPS * dilation // s
        full = ctxs[g].shape[1] - m
        geo.append((s, m, halo, full))

    for g in range(2 if swap else 3):
        s, m, halo, full = geo[g]
        for p in range(s):
            ctxs[g][p, 0:full, :] = jnp.zeros((full, 2 * cols), jnp.bfloat16)

    barrier = pltpu.get_barrier_semaphore()
    if swap:
        for k in range(1, n_sp):
            pl.semaphore_signal(
                barrier, inc=1, device_id={"sp": lax.rem(me + k, n_sp)}, device_id_type=MESH)
    for by in () if swap else (1, 2):
        @pl.when(me >= by)
        def _():
            pl.semaphore_signal(barrier, inc=1, device_id={"sp": me - by}, device_id_type=MESH)
        @pl.when(me + by < n_sp)
        def _():
            pl.semaphore_signal(barrier, inc=1, device_id={"sp": me + by}, device_id_type=MESH)
    for k in range(1, n_tp):
        pl.semaphore_signal(barrier, inc=1, device_id={"tp": lax.rem(tp + k, n_tp)}, device_id_type=MESH)

    loads["tok"].wait()
    loads["gain"].wait()
    part = 32
    @pl.loop(0, rows // part)
    def _(j):
        at = pl.ds(pl.multiple_of(j * part, part), part)
        x = tok[at, :].astype(jnp.float32)
        scale = lax.rsqrt(jnp.mean(x * x, axis=-1, keepdims=True) + 1e-06)
        normed[at, :] = (x * scale * gain[...]).astype(jnp.bfloat16)

    NT = (((1,), (1,)), ((), ()))

    def key_value(g):
        s, m, halo, full = geo[g]
        loads["k", g].wait()
        loads["v", g].wait()
        both = lax.dot_general(
            normed[...], w_all[g, cols:3 * cols, :], NT, preferred_element_type=jnp.float32
        )
        if s == 1:
            ctxs[g][0, full:full + m, :] = both.astype(jnp.bfloat16)
            return
        acc[0, :, 0:cols] = both[:, 0:cols]
        acc[1, :, 0:cols] = both[:, cols:2 * cols]
        for p in range(s):
            for c in range(2):
                piece = acc[c, pl.ds(p, m, stride=s), :]
                ctxs[g][p, full:full + m, c * cols:(c + 1) * cols] = piece[:, 0:cols].astype(jnp.bfloat16)

    def query(g):
        s, m, halo, full = geo[g]
        loads["q", g].wait()
        got = lax.dot_general(
            normed[...], w_all[g, 0:cols, :], NT, preferred_element_type=jnp.float32
        )
        scale = 1.0 / math.sqrt(HEAD_DIM)
        if s == 1:
            queries[g][0] = got.astype(jnp.bfloat16) * jnp.bfloat16(scale)
            return
        acc[0, :, 0:cols] = got
        for p in range(s):
            piece = acc[0, pl.ds(p, m, stride=s), :]
            queries[g][p] = piece[:, 0:cols].astype(jnp.bfloat16) * jnp.bfloat16(scale)

    def region(g, back, streams, last=None):
        s, m, halo, full = geo[g]
        unit = m if g else STEPS
        stop = full - (back - 1) * unit if back else full + m
        size = unit if last is None else last
        return ctxs[g].at[streams, stop - size:stop, :]

    def z_copy(g, src, dst, slot, streams, last=None):
        return pltpu.make_async_remote_copy(
            region(g, src, streams, last), region(g, dst, streams, last),
            zs.at[slot], zr.at[slot], device_id={"sp": me + 2}, device_id_type=MESH)

    def y_copy(g, src, dst, slot, streams):
        return pltpu.make_async_remote_copy(
            region(g, src, streams), region(g, dst, streams),
            ys.at[slot], yr.at[slot], device_id={"sp": partner}, device_id_type=MESH)

    def on(cond, f):
        @pl.when(cond)
        def _():
            f()

    s3 = geo[2][0]
    per = s3 // CHUNKS
    full2 = pl.ds(0, geo[1][0])
    full1 = pl.ds(0, 1)
    tail3 = geo[2][2] - 5 * geo[2][1]
    tail2 = geo[1][2] - geo[1][1]
    z_list = []
    y_list = []
    for k in range(3):
        for c in range(CHUNKS):
            streams = pl.ds(c * per, per)
            z_list.append((2, 2 * k, k * CHUNKS + c, streams, tail3 if k == 2 else None))
            y_list.append((2, 2 * k, k * CHUNKS + c, streams))
    z_list += [(1, 0, 3 * CHUNKS, full2, tail2), (0, 0, 3 * CHUNKS + 1, full1, 0)]
    y_list += [(1, 0, 3 * CHUNKS, full2), (0, 0, 3 * CHUNKS + 1, full1)]

    def z_each(entry, has, act):
        g, src, slot, streams, tail = entry
        if tail is None:
            on(has, lambda: act(z_copy(g, src, src + 2, slot, streams)))
        else:
            if tail:
                on(has & even, lambda: act(z_copy(g, src, src + 2, slot, streams, tail)))
            on(has & odd, lambda: act(z_copy(g, src, src + 2, slot, streams)))

    def z_start(entry):
        z_each(entry, (me >= entry[1]) & (me + 2 < n_sp), lambda c: c.start())

    def z_sent(entry):
        z_each(entry, (me >= entry[1]) & (me + 2 < n_sp), lambda c: c.wait_send())

    def z_recv(entry):
        z_each(entry, me >= entry[1] + 2, lambda c: c.wait_recv())

    def y_even(entry, act):
        g, src, slot, streams = entry
        on(even & (me >= src), lambda: act(y_copy(g, src, src + 1, slot, streams)))

    def y_odd(entry, act):
        g, src, slot, streams = entry
        on(odd & (me >= src + 2), lambda: act(y_copy(g, src + 2, src + 1, slot, streams)))

    def y_recv(entry):
        g, src, slot, streams = entry
        on(me >= src + 1, lambda: y_copy(g, src, src + 1, slot, streams).wait_recv())

    start = lambda c: c.start()
    sent = lambda c: c.wait_send()
    z3 = lambda k: z_list[k * CHUNKS:(k + 1) * CHUNKS]
    y3 = lambda k: y_list[k * CHUNKS:(k + 1) * CHUNKS]

    def whole_stream():
        s, m, halo, full = geo[2]
        for name in "qkv":
            loads[name, 2].wait()
        got = lax.dot_general(normed[...], w_all[2], NT, preferred_element_type=jnp.float32)
        for c in range(3):
            acc[c] = got[:, c * cols:(c + 1) * cols]
        for p in range(s):
            for c in range(3):
                piece = acc[c, pl.ds(p, m, stride=s), :].astype(jnp.bfloat16)
                if c == 0:
                    piece = piece * jnp.bfloat16(1.0 / math.sqrt(HEAD_DIM))
                going[p, :, c * cols:(c + 1) * cols] = piece

    per_dev = geo[2][1]

    def mine_at(e):
        return pl.ds(pl.multiple_of(e * per_dev, 16), per_dev)

    def go(e, source):
        return pltpu.make_async_remote_copy(
            going.at[e], stream.at[mine_at(source), :], gs.at[e], gr.at[source],
            device_id={"sp": e}, device_id_type=MESH)

    def reply(e, source):
        return pltpu.make_async_remote_copy(
            answer.at[e * per_dev:(e + 1) * per_dev, :], back.at[source], bs.at[e], br.at[source],
            device_id={"sp": e}, device_id_type=MESH)

    def go_arrival(source):
        pltpu.make_async_remote_copy(
            going.at[source], stream.at[mine_at(source), :], gs.at[source], gr.at[source],
            device_id={"sp": source}, device_id_type=MESH).wait_recv()

    def reply_arrival(source):
        pltpu.make_async_remote_copy(
            answer.at[source * per_dev:(source + 1) * per_dev, :], back.at[source],
            bs.at[source], br.at[source],
            device_id={"sp": source}, device_id_type=MESH).wait_recv()

    def each_peer(f, peers=None):
        for e in peers or range(n_sp):
            on(me != e, lambda: f(e))

    if swap:
        whole_stream()
    else:
        key_value(2)
    if swap:
        peers = n_sp - 1 + n_tp - 1
    else:
        peers = jnp.minimum(me, 2) + jnp.minimum(n_sp - 1 - me, 2) + (n_tp - 1)
    pl.semaphore_wait(barrier, peers)
    if swap:
        each_peer(lambda e: go(e, me).start())
        stream[mine_at(me), :] = going[me]
    else:
        for c in range(CHUNKS):
            z_start(z3(0)[c])
            y_even(y3(0)[c], start)
    def near(entry):
        g, by, slot, last = entry
        streams = full2 if g else full1
        return pltpu.make_async_remote_copy(
            region(g, 0, streams, last), region(g, by, streams, last),
            zs.at[slot], zr.at[slot], device_id={"sp": me + by}, device_id_type=MESH)

    def near_start(entry):
        on(me + entry[1] < n_sp, lambda: near(entry).start())

    def near_sent(entry):
        on(me + entry[1] < n_sp, lambda: near(entry).wait_send())

    def near_recv(entry):
        on(me >= entry[1], lambda: near(entry).wait_recv())

    near_list = [(0, 1, 0, None), (1, 1, 1, None), (1, 2, 2, tail2)]
    if swap:
        key_value(0)
        near_start(near_list[0])
        key_value(1)
        near_start(near_list[1])
        near_start(near_list[2])
    else:
        key_value(1)
        z_start(z_list[-2])
        y_even(y_list[-2], start)
        key_value(0)
        z_start(z_list[-1])
        y_even(y_list[-1], start)
    for g in (0, 1) if swap else (0, 1, 2):
        query(g)

    def relay(k):
        for c in range(CHUNKS):
            z_recv(z3(k - 1)[c])
            z_start(z3(k)[c])
            y_odd(y3(k - 1)[c], start)
            y_even(y3(k)[c], start)

    lane_head = lax.broadcasted_iota(jnp.int32, (1, cols), 1) // HEAD_DIM

    def bias_of(g, height, length, first_key, offset):
        s = geo[g][0]
        halo = geo[g][2]
        ratio = DILATIONS[g] // s
        row = lax.broadcasted_iota(jnp.int32, (height, length), 0)
        col = lax.broadcasted_iota(jnp.int32, (height, length), 1)
        apart = row + offset - col
        step = apart // ratio
        valid = (apart >= 0) & (apart <= STEPS * ratio)
        if ratio > 1:
            valid = valid & (apart % ratio == 0)
        valid = valid & ((col + first_key) * s >= halo * s - me * rows)
        parts = []
        for h in range(heads):
            slot = (g * total_slots + tp * heads + h + 1).astype(jnp.float32)
            slope = jnp.exp2(jnp.full((1, 1), -8.0 / (3 * total_slots), jnp.float32) * slot)
            parts.append(jnp.where(valid, -slope * step.astype(jnp.float32), NEG_BIG))
        return jnp.concatenate(parts, axis=0) if heads > 1 else parts[0]

    def attend(q, keys, values, bias):
        height = q.shape[0]
        stacked = [jnp.where(lane_head == h, q, jnp.zeros_like(q)) for h in range(heads)]
        stacked = jnp.concatenate(stacked, axis=0) if heads > 1 else stacked[0]
        logits = lax.dot_general(stacked, keys, NT, preferred_element_type=jnp.float32) + bias
        top = jnp.max(logits, axis=-1, keepdims=True)
        e = jnp.exp(logits - top)
        total = jnp.sum(e, axis=-1, keepdims=True)
        lse = top + jnp.log(total)
        weights = (e * (1.0 / total)).astype(jnp.bfloat16)
        o = jnp.dot(weights, values, preferred_element_type=jnp.float32)
        out = o[0:height]
        log = jnp.broadcast_to(lse[0:height], (height, cols))
        for h in range(1, heads):
            mine = lane_head == h
            out = jnp.where(mine, o[h * height:(h + 1) * height], out)
            log = jnp.where(mine, lse[h * height:(h + 1) * height], log)
        return out, log

    def put(g, at, out, log):
        if cols < wide:
            out = jnp.concatenate([out] * (wide // cols), axis=1)
            log = jnp.concatenate([log] * (wide // cols), axis=1)
        outs[g, at, :] = out
        lses[g, at, :] = log

    def attend_group(g, first, count):
        s, m, halo, full = geo[g]
        base = full - halo
        bias = bias_of(g, m, halo + m, 0, halo)
        for p in range(first, first + count):
            out, log = attend(
                queries[g][p], ctxs[g][p, base:full + m, 0:cols],
                ctxs[g][p, base:full + m, cols:2 * cols], bias)
            put(g, pl.ds(p, m, stride=s), out, log)

    tile = STEPS

    def near_tile(j):
        base = geo[0][3] - STEPS + j * tile
        bias = bias_of(0, tile, tile + STEPS, j * tile, STEPS)
        out, log = attend(
            qs1[0, j * tile:(j + 1) * tile, :], ctx1[0, base:base + tile + STEPS, 0:cols],
            ctx1[0, base:base + tile + STEPS, cols:2 * cols], bias)
        put(0, pl.ds(j * tile, tile), out, log)

    def pass_on(entry, y_entry):
        z_recv(entry)
        y_odd(y_entry, start)

    same_head = (
        lax.broadcasted_iota(jnp.int32, (cols, cols), 0) // HEAD_DIM
        == lax.broadcasted_iota(jnp.int32, (cols, cols), 1) // HEAD_DIM
    ).astype(jnp.bfloat16)

    def stream_tile(j):
        stop = (j + 1) * tile
        s = geo[2][0]
        ratio = DILATIONS[2] // s
        row = lax.broadcasted_iota(jnp.int32, (tile, stop), 0)
        col = lax.broadcasted_iota(jnp.int32, (tile, stop), 1)
        apart = row + j * tile - col
        valid = (apart >= 0) & (apart <= STEPS * ratio) & (apart % ratio == 0)
        parts = []
        for h in range(heads):
            slot = (2 * total_slots + tp * heads + h + 1).astype(jnp.float32)
            slope = jnp.exp2(jnp.full((1, 1), -8.0 / (3 * total_slots), jnp.float32) * slot)
            parts.append(jnp.where(valid, -slope * (apart // ratio).astype(jnp.float32), NEG_BIG))
        bias = jnp.concatenate(parts, axis=0) if heads > 1 else parts[0]
        out, log = attend(
            stream[j * tile:stop, 0:cols], stream[0:stop, cols:2 * cols],
            stream[0:stop, 2 * cols:3 * cols], bias)
        high = log.astype(jnp.bfloat16).astype(jnp.float32)
        mid = (log - high).astype(jnp.bfloat16).astype(jnp.float32)
        low = log - high - mid
        place = lax.rem(lax.broadcasted_iota(jnp.int32, (1, cols), 1), HEAD_DIM)
        terms = jnp.where(place == 0, high, jnp.where(place == 1, mid, jnp.where(place == 2, low, 0.0)))
        answer[j * tile:stop, 0:cols] = out.astype(jnp.bfloat16)
        answer[j * tile:stop, cols:2 * cols] = terms.astype(jnp.bfloat16)

    if swap:
        for j in range(1, rows // tile):
            near_tile(j)
        each_peer(lambda e: go_arrival(e))
        done = 0
        for j in range(rows // tile):
            stream_tile(j)
            ready = (j + 1) * tile // per_dev
            each_peer(lambda e: reply(e, me).start(), range(done, ready))
            done = ready
        back[me] = answer[mine_at(me), :]
        near_recv(near_list[0])
        near_tile(0)
        near_recv(near_list[1])
        near_recv(near_list[2])
        attend_group(1, 0, geo[1][0])
        each_peer(lambda e: reply_arrival(e))
        for e in range(n_sp):
            log = jnp.dot(back[e, :, cols:2 * cols], same_head, preferred_element_type=jnp.float32)
            put(2, pl.ds(e, per_dev, stride=n_sp), back[e, :, 0:cols].astype(jnp.float32), log)
    else:
        relay(1)
        pass_on(z_list[-2], y_list[-2])
        pass_on(z_list[-1], y_list[-1])
        y_recv(y_list[-1])
        for j in range(rows // tile):
            near_tile(j)
        relay(2)
        y_recv(y_list[-2])
        attend_group(1, 0, geo[1][0])
        for c in range(CHUNKS):
            pass_on(z3(2)[c], y3(2)[c])
        for c in range(CHUNKS):
            for k in range(3):
                y_recv(y3(k)[c])
            attend_group(2, c * per, per)

    for j in range(rows // tile):
        at = pl.ds(j * tile, tile)
        logs = [lses[g, at, :] for g in range(3)]
        top = jnp.maximum(jnp.maximum(logs[0], logs[1]), logs[2])
        lw = top + jnp.log(sum(jnp.exp(l - top) for l in logs))
        mixed = sum(jnp.exp(logs[g] - lw) * outs[g, at, :] for g in range(3))
        mix[tp, at, :] = mixed[:, 0:cols].astype(jnp.bfloat16)
        flipped = lw.T
        for h in range(heads):
            logw_ref[h:h + 1, j * tile:(j + 1) * tile] = flipped[h * HEAD_DIM:h * HEAD_DIM + 1, :]

    def spread(k):
        to = lax.rem(tp + k, n_tp)
        return pltpu.make_async_remote_copy(
            mix.at[tp], mix.at[tp], ms.at[k - 1], mr.at[k - 1],
            device_id={"tp": to}, device_id_type=MESH)

    def arrival(k):
        source = lax.rem(tp + n_tp - k, n_tp)
        return pltpu.make_async_remote_copy(
            mix.at[source], mix.at[source], ms.at[k - 1], mr.at[k - 1],
            device_id={"tp": lax.rem(tp + k, n_tp)}, device_id_type=MESH)

    for k in range(1, n_tp):
        spread(k).start()
    for k in range(1, n_tp):
        arrival(k).wait_recv()
    for t in range(n_tp):
        every_ref[:, t * cols:(t + 1) * cols] = mix[t]

    for k in range(1, n_tp):
        spread(k).wait_send()
    if swap:
        each_peer(lambda e: go(e, me).wait_send())
        each_peer(lambda e: reply(e, me).wait_send())
        for entry in near_list:
            near_sent(entry)
    for entry in () if swap else z_list:
        z_sent(entry)
    for entry in () if swap else y_list:
        y_even(entry, sent)
        y_odd(entry, sent)


LANES = 128
NT = (((1,), (1,)), ((), ()))


def split_kernel(
    n_sp, n_tp, total_slots,
    tok_hbm, gain_hbm, wq_hbm, wk_hbm, wv_hbm, wo_hbm,
    proj_ref, logw_ref,
    tok, gain, w_all, w_out, normed, acc, q1, q2, ctx1, ctx2, going, stream, qfar,
    answer, answer_far, lse_near, lse_far, back, back_far, back_lse, back_far_lse,
    b0, b0_first, b1, b2, b3, out0, log0, part_o, part_l, mix, nat, flat, lw_nat,
    in_sem, one, ns, nr, br, cr, xr, dr, er,
):
    rows, width = tok.shape
    cols = wq_hbm.shape[1]
    heads = cols // HEAD_DIM
    classes = going.shape[0]
    per = rows // classes
    ratio = DILATIONS[2] // classes
    tile = STEPS
    me = lax.axis_index("sp")
    tp = lax.axis_index("tp")
    mine = lax.rem(me, classes)
    base = me - mine
    upper = me >= classes
    lower = me < classes

    gs, gr, fs, fr, as_, ar, ls, lr, bs, cs, xs, ds, es = [one.at[n] for n in range(13)]
    loads = {}

    def load(name, src, dst, sem):
        loads[name] = pltpu.make_async_copy(src, dst, in_sem.at[sem])
        loads[name].start()

    for c in range(classes):
        at = pl.ds(c * per, per)
        load(("tok", c), tok_hbm.at[at], tok.at[at], c)
        if c == 0:
            load("gain", gain_hbm, gain, classes)
    weights = (
        (2, "q"), (2, "k"), (2, "v"), (1, "k"), (1, "v"), (0, "k"), (0, "v"), (1, "q"), (0, "q"))
    for slot, (g, kind) in enumerate(weights):
        src = {"q": wq_hbm, "k": wk_hbm, "v": wv_hbm}[kind]
        sem = classes + (1 if slot < 3 else 2 if slot < 7 else 3)
        load((kind, g), src.at[g], w_all.at[slot * cols:(slot + 1) * cols], sem)
    load("out", wo_hbm, w_out, classes + 4)

    barrier = pltpu.get_barrier_semaphore()
    for k in range(1, n_sp):
        pl.semaphore_signal(
            barrier, inc=1, device_id={"sp": lax.rem(me + k, n_sp)}, device_id_type=MESH)
    for k in range(1, n_tp):
        pl.semaphore_signal(
            barrier, inc=1, device_id={"tp": lax.rem(tp + k, n_tp)}, device_id_type=MESH)

    @pl.when(me == 0)
    def _():
        ctx1[0:tile, :] = jnp.zeros((tile, 2 * cols), jnp.bfloat16)
        for p in range(classes):
            ctx2[p, 0:tile, :] = jnp.zeros((tile, 2 * cols), jnp.bfloat16)

    @pl.when(me == 1)
    def _():
        for p in range(classes):
            ctx2[p, 0:tile - per, :] = jnp.zeros((tile - per, 2 * cols), jnp.bfloat16)

    def bias(g, height, first, last, offset, step, key_limit):
        row = lax.broadcasted_iota(jnp.int32, (height, last - first), 0)
        col = lax.broadcasted_iota(jnp.int32, (height, last - first), 1) + first
        apart = row + offset - col
        valid = (apart >= 0) & (apart <= STEPS * step)
        shift = step.bit_length() - 1
        if step > 1:
            valid = valid & ((apart & (step - 1)) == 0)
        if key_limit is not None:
            valid = valid & (col >= key_limit)
        far = lax.shift_right_arithmetic(apart, shift).astype(jnp.float32)
        parts = []
        for h in range(heads):
            slot = (g * total_slots + tp * heads + h + 1).astype(jnp.float32)
            slope = jnp.exp2(jnp.full((1, 1), -8.0 / (3 * total_slots), jnp.float32) * slot)
            parts.append(jnp.where(valid, -slope * far, NEG_BIG))
        return parts

    def keep(ref, parts):
        height, length = parts[0].shape
        for h in range(heads):
            ref[h * height:(h + 1) * height, 0:length] = parts[h]

    def near_keys(k):
        return -(-(k + 1) * per // LANES) * LANES

    def far_keys(k):
        return max(0, (rows + k * per - STEPS * ratio) // LANES * LANES)

    keep(b0, bias(0, tile, 0, 2 * tile, tile, 1, None))
    keep(b0_first, bias(0, tile, 0, 2 * tile, tile, 1, jnp.where(me == 0, tile, 0)))
    keep(b1, bias(1, per, 0, tile + per, tile, 1, jnp.maximum(tile - me * per, 0)))
    for k in range(classes):
        keep(b2.at[k], bias(2, per, 0, near_keys(k), k * per, ratio, None))
        keep(b3.at[k], bias(2, per, far_keys(k), rows, rows + k * per, ratio, None))

    loads["gain"].wait()
    part = 32
    for c in range(classes):
        loads["tok", c].wait()
        for j in range(per // part):
            at = pl.ds(c * per + j * part, part)
            x = tok[at, :].astype(jnp.float32)
            scale = lax.rsqrt(jnp.mean(x * x, axis=-1, keepdims=True) + 1e-06)
            normed[at, :] = (x * scale * gain[...]).astype(jnp.bfloat16)

    def product(first, count, sem):
        part = w_all.at[first * cols:(first + count) * cols]
        pltpu.make_async_copy(part, part, in_sem.at[classes + sem]).wait()
        return lax.dot_general(
            normed[...], part[...], NT, preferred_element_type=jnp.float32)

    def by_class(n, p):
        return acc[n, pl.ds(p, per, stride=classes), :].astype(jnp.bfloat16)

    scaling = jnp.bfloat16(1.0 / math.sqrt(HEAD_DIM))
    got = product(0, 3, 1)
    for n in range(3):
        acc[n] = got[:, n * cols:(n + 1) * cols]
    for p in range(classes):
        going[p, :, 0:cols] = by_class(0, p) * scaling
        going[p, :, cols:2 * cols] = by_class(1, p)
        going[p, :, 2 * cols:3 * cols] = by_class(2, p)

    def slice_of(k):
        return pl.ds(pl.multiple_of(k * per, 16), per)

    def remote(src, dst, send, recv, sp):
        return pltpu.make_async_remote_copy(
            src, dst, send, recv, device_id={"sp": sp}, device_id_type=MESH)

    def go(c, source):
        return remote(going.at[c], stream.at[slice_of(source), :], gs, gr, base + c)

    def go_far(c, source):
        return remote(going.at[c, :, 0:cols], qfar.at[source], fs, fr, c)

    def reply(e, source):
        return remote(answer.at[e], back.at[source], as_, ar, base + e)

    def reply_lse(e, source):
        return remote(lse_near.at[e], back_lse.at[source], ls, lr, base + e)

    def reply_far(e, source):
        return remote(
            answer_far.at[e], back_far.at[source], bs, br.at[source], classes + e)

    def reply_far_lse(e, source):
        return remote(
            lse_far.at[e], back_far_lse.at[source], cs, cr.at[source], classes + e)

    def when(cond, f):
        @pl.when(cond)
        def _():
            f()

    def each_peer(f):
        for e in range(classes):
            when(mine != e, lambda: f(e))

    tail = tile - per
    full2 = pl.ds(0, classes)

    even = lax.rem(me, 2) == 0
    odd = lax.rem(me, 2) == 1

    def near(n):
        if n == 0:
            src, dst, by = ctx1.at[rows:rows + tile, :], ctx1.at[0:tile, :], 1
        elif n == 1:
            src, dst, by = ctx2.at[full2, tile:tile + per, :], ctx2.at[full2, tail:tile, :], 1
        else:
            src, dst, by = ctx2.at[full2, tile + per - tail:tile + per, :], ctx2.at[full2, 0:tail, :], 2
        return remote(src, dst, ns.at[n], nr.at[n], me + by)

    sends = (me + 1 < n_sp, me + 1 < n_sp, me + 2 < n_sp)
    gets = (me >= 1, me >= 1, me >= 2)

    def near_start(n, side):
        when(sends[n] & side, near(n).start)

    def near_sent(n):
        when(sends[n], near(n).wait_send)

    def near_arrival(n):
        when(gets[n], near(n).wait_recv)

    pl.semaphore_wait(barrier, n_sp - 1 + n_tp - 1)

    @pl.when(upper)
    def _():
        for c in range(classes):
            go_far(c, mine).start()

    each_peer(lambda e: go(e, mine).start())
    stream[slice_of(mine), :] = going[mine]

    got = product(3, 4, 2)
    for n in range(2):
        acc[n] = got[:, n * cols:(n + 1) * cols]
    for p in range(classes):
        for n in range(2):
            ctx2[p, tile:tile + per, n * cols:(n + 1) * cols] = by_class(n, p)
    ctx1[tile:tile + rows, :] = got[:, 2 * cols:4 * cols].astype(jnp.bfloat16)

    got = product(7, 2, 3)
    acc[2] = got[:, 0:cols]
    for p in range(classes):
        q2[p] = by_class(2, p) * scaling
    q1[...] = got[:, cols:2 * cols].astype(jnp.bfloat16) * scaling
    near_start(1, even)
    near_start(2, even)
    near_start(0, even)

    lane = lax.broadcasted_iota(jnp.int32, (1, cols), 1)
    lane_head = lane // HEAD_DIM
    lane_turn = lax.rem(lane, heads)

    def attend(q, keys, values, bias_ref, length):
        height = q.shape[0]
        stacked = jnp.concatenate(
            [jnp.where(lane_head == h, q, jnp.zeros_like(q)) for h in range(heads)], axis=0)
        logits = lax.dot_general(stacked, keys, NT, preferred_element_type=jnp.float32)
        logits = logits + bias_ref[0:heads * height, 0:length]
        top = jnp.max(logits, axis=-1, keepdims=True)
        e = jnp.exp(logits - top)
        total = jnp.sum(e, axis=-1, keepdims=True)
        o = jnp.dot(e.astype(jnp.bfloat16), values, preferred_element_type=jnp.float32)
        o = o * (1.0 / total)
        lse = top + jnp.log(total)
        out = o[0:height]
        for h in range(1, heads):
            out = jnp.where(lane_head == h, o[h * height:(h + 1) * height], out)
        return out, [lse[h * height:(h + 1) * height] for h in range(heads)]

    def lanes_of(lse, pattern):
        log = jnp.broadcast_to(lse[0], (lse[0].shape[0], cols))
        for h in range(1, heads):
            log = jnp.where(pattern == h, lse[h], log)
        return log

    def pack(ref, k, lse):
        ref[k, :, 0:per] = lanes_of(lse, lane_turn).T[0:heads, :]

    def unpack(ref, k):
        row = ref[k]
        wide = [jnp.broadcast_to(row[h:h + 1, :], (HEAD_DIM, LANES)) for h in range(heads)]
        return jnp.concatenate(wide, axis=0).T[0:per, :]

    def near_tile(j, bias_ref):
        first = j * tile
        out, lse = attend(
            q1[first:first + tile, :], ctx1[first:first + 2 * tile, 0:cols],
            ctx1[first:first + 2 * tile, cols:2 * cols], bias_ref, 2 * tile)
        out0[first:first + tile, :] = out
        log0[first:first + tile, :] = lanes_of(lse, lane_head)

    for j in range(1, rows // tile):
        near_tile(j, b0)
    near_start(2, odd)
    near_start(1, odd)
    near_start(0, odd)

    others = classes - 1

    def wait_bytes(ref, sem):
        pltpu.make_async_copy(ref, ref, sem).wait()

    wait_bytes(stream.at[0:others * per, :], gr)
    for k in range(classes):
        stop = near_keys(k)
        out, lse = attend(
            stream[k * per:(k + 1) * per, 0:cols], stream[0:stop, cols:2 * cols],
            stream[0:stop, 2 * cols:3 * cols], b2.at[k], stop)
        answer[k] = out.astype(jnp.bfloat16)
        pack(lse_near, k, lse)
    each_peer(lambda e: (reply(e, mine).start(), reply_lse(e, mine).start()))
    back[mine] = answer[mine]
    back_lse[mine] = lse_near[mine]

    @pl.when(lower)
    def _():
        wait_bytes(qfar, fr)
        for k in range(classes):
            first = far_keys(k)
            out, lse = attend(
                qfar[k], stream[first:rows, cols:2 * cols],
                stream[first:rows, 2 * cols:3 * cols], b3.at[k], rows - first)
            answer_far[k] = out.astype(jnp.bfloat16)
            pack(lse_far, k, lse)
        for k in range(classes):
            turn = lax.rem(mine + k, classes)
            reply_far(turn, mine).start()
            reply_far_lse(turn, mine).start()

    for n in range(3):
        near_arrival(n)
    near_tile(0, b0_first)
    near_parts = []
    for p in range(classes):
        near_parts.append(attend(
            q2[p], ctx2[p, :, 0:cols], ctx2[p, :, cols:2 * cols], b1, tile + per))
    for p in range(classes):
        out, lse = near_parts[p]
        part_o[p] = out
        part_l[p] = lanes_of(lse, lane_head)

    def merge(logs, outs):
        top = functools.reduce(jnp.maximum, logs)
        log = top + jnp.log(sum(jnp.exp(l - top) for l in logs))
        return log, sum(jnp.exp(l - log) * o for l, o in zip(logs, outs))

    wait_bytes(back.at[0:others], ar)
    wait_bytes(back_lse.at[0:others], lr)
    for p in range(classes):
        at = pl.ds(p, per, stride=classes)
        log, out = merge(
            [log0[at, :], part_l[p], unpack(back_lse, p)],
            [out0[at, :], part_o[p], back[p].astype(jnp.float32)])
        part_l[p] = log
        part_o[p] = out
    turns = [lax.rem(mine + classes - k, classes) for k in range(classes)]

    mate = tp + 1 - 2 * lax.rem(tp, 2)
    across = lax.rem(tp + n_tp // 2, n_tp)

    def hand(source, c, to, send, recv):
        return pltpu.make_async_remote_copy(
            mix.at[source, c], mix.at[source, c], send, recv.at[c],
            device_id={"tp": to}, device_id_type=MESH)

    first_core = lax.rem(tp, 2) == 0
    across_mate = lax.rem(mate + n_tp // 2, n_tp)

    def finish(c):
        @pl.when(upper)
        def _():
            reply_far(c, c).wait_recv()
            reply_far_lse(c, c).wait_recv()
            log, out = merge(
                [part_l[c], unpack(back_far_lse, c)],
                [part_o[c], back_far[c].astype(jnp.float32)])
            part_l[c] = log
            part_o[c] = out

        mix[tp, c] = part_o[c].astype(jnp.bfloat16)

        @pl.when(first_core)
        def _():
            hand(tp, c, across_mate, es, er).start()

        hand(tp, c, across, xs, xr).start()
        hand(tp, c, mate, ds, dr).start()

    def forward(c):
        @pl.when(~first_core)
        def _():
            hand(across, c, across, xs, xr).wait_recv()
            hand(across, c, mate, ds, dr).start()

    def project_class(c):
        @pl.when(first_core)
        def _():
            hand(across, c, across, xs, xr).wait_recv()
            wait_bytes(mix.at[0:2, 0], dr.at[c])

        @pl.when(~first_core)
        def _():
            hand(across, c, across, es, er).wait_recv()
            wait_bytes(mix.at[0, 0], dr.at[c])
        mixed = jnp.concatenate([mix[t, c] for t in range(n_tp)], axis=1)
        got = jnp.dot(mixed, w_out[...], preferred_element_type=jnp.float32)
        for n in range(nat.shape[0]):
            nat[n, c] = got[:, n * LANES:(n + 1) * LANES]

    for c in turns:
        finish(c)
    loads["out"].wait()
    for p in range(classes):
        lw_nat[pl.ds(p, per, stride=classes), :] = part_l[p]
    for c in turns:
        forward(c)
    for c in turns:
        project_class(c)
    for n in range(nat.shape[0]):
        for p in range(classes):
            flat[n, pl.ds(p, per, stride=classes), :] = nat[n, p]
        proj_ref[:, n * LANES:(n + 1) * LANES] = flat[n].astype(jnp.bfloat16)
    for j in range(rows // tile):
        flipped = lw_nat[j * tile:(j + 1) * tile, :].T
        for h in range(heads):
            logw_ref[h:h + 1, j * tile:(j + 1) * tile] = flipped[h * HEAD_DIM:h * HEAD_DIM + 1, :]

    wait_bytes(mix.at[0], xs)

    @pl.when(first_core)
    def _():
        wait_bytes(mix.at[0], ds)
        wait_bytes(mix.at[0], es)

    @pl.when(~first_core)
    def _():
        wait_bytes(mix.at[0:2], ds)

    wait_bytes(going.at[0:others], gs)
    wait_bytes(answer.at[0:others], as_)
    wait_bytes(lse_near.at[0:others], ls)

    @pl.when(upper)
    def _():
        wait_bytes(going.at[:, :, 0:cols], fs)

    @pl.when(lower)
    def _():
        wait_bytes(answer_far, bs)
        wait_bytes(lse_far, cs)

    for n in range(3):
        near_sent(n)


def store(proj_ref, logw_ref, proj_out, logw_out, sem):
    copies = [
        pltpu.make_async_copy(proj_ref, proj_out, sem.at[0]),
        pltpu.make_async_copy(logw_ref, logw_out, sem.at[1]),
    ]
    for copy in copies:
        copy.start()
    for copy in copies:
        copy.wait()


def split_call(n_sp, n_tp, tokens, norm_gain, w_query, w_key, w_value, w_out):
    rows, width = tokens.shape
    cols = w_query.shape[1]
    out_cols = w_out.shape[1]
    heads = cols // HEAD_DIM
    classes = n_sp // 2
    per = rows // classes
    bf, f32 = jnp.bfloat16, jnp.float32
    vmem = pltpu.VMEM
    dma = pltpu.SemaphoreType.DMA
    lanes2 = heads * per
    shapes = (
        jax.ShapeDtypeStruct((rows, out_cols), bf),
        jax.ShapeDtypeStruct((heads, rows), f32),
    )
    results = pl.pallas_call(
        functools.partial(split_kernel, n_sp, n_tp, heads * n_tp),
        out_shape=tuple(vmem(shape.shape, shape.dtype) for shape in shapes),
        in_specs=[pl.BlockSpec(memory_space=pltpu.HBM)] * 6,
        out_specs=(pl.BlockSpec(memory_space=pltpu.VMEM),) * 2,
        scratch_shapes=[
            vmem((rows, width), bf),
            vmem((1, width), f32),
            vmem((9 * cols, width), bf),
            vmem(w_out.shape, bf),
            vmem((rows, width), bf),
            vmem((3, rows, cols), f32),
            vmem((rows, cols), bf),
            vmem((classes, per, cols), bf),
            vmem((STEPS + rows, 2 * cols), bf),
            vmem((classes, STEPS + per, 2 * cols), bf),
            vmem((classes, per, 3 * cols), bf),
            vmem((rows, 3 * cols), bf),
            vmem((classes, per, cols), bf),
            vmem((classes, per, cols), bf),
            vmem((classes, per, cols), bf),
            vmem((classes, heads, LANES), f32),
            vmem((classes, heads, LANES), f32),
            vmem((classes, per, cols), bf),
            vmem((classes, per, cols), bf),
            vmem((classes, heads, LANES), f32),
            vmem((classes, heads, LANES), f32),
            vmem((heads * STEPS, 2 * STEPS), f32),
            vmem((heads * STEPS, 2 * STEPS), f32),
            vmem((lanes2, STEPS + per), f32),
            vmem((classes, lanes2, rows), f32),
            vmem((classes, lanes2, rows), f32),
            vmem((rows, cols), f32),
            vmem((rows, cols), f32),
            vmem((classes, per, cols), f32),
            vmem((classes, per, cols), f32),
            vmem((n_tp, classes, per, cols), bf),
            vmem((out_cols // LANES, classes, per, LANES), f32),
            vmem((out_cols // LANES, rows, LANES), f32),
            vmem((rows, cols), f32),
            dma((classes + 5,)), dma((13,)), dma((3,)), dma((3,)),
            dma((classes,)), dma((classes,)), dma((classes,)), dma((classes,)), dma((classes,)),
        ],
        compiler_params=pltpu.CompilerParams(
            collective_id=0, has_side_effects=True, vmem_limit_bytes=VMEM_LIMIT
        ),
    )(tokens, norm_gain.reshape(1, width), w_query, w_key, w_value, w_out)
    return pl.pallas_call(
        store,
        out_shape=shapes,
        in_specs=[pl.BlockSpec(memory_space=pltpu.VMEM)] * 2,
        out_specs=(pl.BlockSpec(memory_space=pl.ANY),) * 2,
        scratch_shapes=[pltpu.SemaphoreType.DMA((2,))],
        compiler_params=pltpu.CompilerParams(vmem_limit_bytes=STORE_LIMIT),
    )(*results)


def splits(n_sp, n_tp, rows, cols, out_cols):
    classes = n_sp // 2
    if n_tp != 4 or n_sp % 2 or classes != DILATIONS[1] or DILATIONS[2] % classes:
        return False
    if cols != LANES or LANES % HEAD_DIM or rows % (classes * 32) or rows % STEPS or out_cols % LANES:
        return False
    per = rows // classes
    window = STEPS * DILATIONS[2] // classes
    return per <= STEPS <= 2 * per and classes * per <= window


def project(every_ref, w_ref, log_ref, proj_ref, logw_ref):
    proj_ref[...] = jnp.dot(
        every_ref[...], w_ref[...], preferred_element_type=jnp.float32
    ).astype(jnp.bfloat16)
    logw_ref[...] = log_ref[...]


def solution(mesh):
    n_sp, n_tp = mesh.shape["sp"], mesh.shape["tp"]

    def per_device(tokens, norm_gain, w_query, w_key, w_value, w_out):
        rows, width = tokens.shape
        cols = w_query.shape[1]
        out_cols = w_out.shape[1]
        heads = cols // HEAD_DIM
        wide = max(cols, 128)
        if splits(n_sp, n_tp, rows, cols, out_cols):
            return split_call(n_sp, n_tp, tokens, norm_gain, w_query, w_key, w_value, w_out)
        bf, f32 = jnp.bfloat16, jnp.float32
        counts = [streams_of(d, rows) for d in DILATIONS]
        m = [rows // s for s in counts]
        slots = 3 * CHUNKS + 2
        swap = n_sp == counts[2] and cols % 128 == 0
        vmem = pltpu.VMEM
        dma = pltpu.SemaphoreType.DMA
        mixed, logs = pl.pallas_call(
            functools.partial(kernel, n_sp, n_tp, heads * n_tp, swap),
            out_shape=(
                jax.ShapeDtypeStruct((rows, n_tp * cols), bf),
                jax.ShapeDtypeStruct((heads, rows), f32),
            ),
            in_specs=[pl.BlockSpec(memory_space=pl.ANY)] * 5,
            out_specs=(pl.BlockSpec(memory_space=pltpu.VMEM),) * 2,
            scratch_shapes=[
                vmem((rows, width), bf),
                vmem((1, width), f32),
                vmem((3, 3 * cols, width), bf),
                vmem((rows, width), bf),
                vmem((3, rows, wide), f32),
                vmem((counts[0], m[0], cols), bf),
                vmem((counts[1], m[1], cols), bf),
                vmem((counts[2], m[2], cols), bf),
                vmem((1, 2 * STEPS + rows, 2 * cols), bf),
                vmem((counts[1], 3 * m[1], 2 * cols), bf),
                vmem((counts[2], 7 * m[2], 2 * cols), bf),
                vmem((3, rows, wide), f32),
                vmem((3, rows, wide), f32),
                vmem((n_tp, rows, cols), bf),
                vmem((counts[2], m[2], 3 * cols), bf),
                vmem((rows, 3 * cols), bf),
                vmem((rows, 2 * cols), bf),
                vmem((counts[2], m[2], 2 * cols), bf),
                dma((12,)),
                dma((slots,)), dma((slots,)), dma((slots,)), dma((slots,)),
                dma((n_tp - 1,)), dma((n_tp - 1,)),
                dma((n_sp,)), dma((n_sp,)), dma((n_sp,)), dma((n_sp,)),
            ],
            compiler_params=pltpu.CompilerParams(
                collective_id=0, has_side_effects=True, vmem_limit_bytes=60 * 1024 * 1024
            ),
        )(tokens, norm_gain.reshape(1, width), w_query, w_key, w_value)
        return pl.pallas_call(
            project,
            out_shape=(
                jax.ShapeDtypeStruct((rows, out_cols), bf),
                jax.ShapeDtypeStruct((heads, rows), f32),
            ),
        )(mixed, w_out, logs)

    in_specs = (
        P("sp", None),
        P(),
        P(None, "tp", None),
        P(None, "tp", None),
        P(None, "tp", None),
        P(None, "tp"),
    )
    out_specs = (P("sp", "tp"), P("tp", "sp"))
    return jax.shard_map(
        per_device, mesh=mesh, in_specs=in_specs, out_specs=out_specs, check_vma=False
    )
```
